32 devices in a mesh: grp: 2 (over y), fs: 4 (over z), tp: 4 (over x, core).
Axes of the slice: x: 2, y: 2, z: 4, core: 2. Of those that a mesh axis runs over, the one named last changes fastest.
Arguments:
- tokens: bfloat16 [3072, 2048], P(('grp', 'fs')), parts along dimension 0, may hold values from -3 to 3
- gate_weight: bfloat16 [2048, 5120], P('fs', 'tp'), may hold values from -0.125 to 0.125
- up_weight: bfloat16 [2048, 5120], P('fs', 'tp'), may hold values from -0.125 to 0.125
- down_weight: bfloat16 [5120, 2048], P('tp', 'fs'), may hold values from -0.078125 to 0.078125
- pool_weight: bfloat16 [512, 4, 512], P('fs', None, 'tp'), may hold values from -0.375 to 0.375
- pool_bias: float32 [4, 512], replicated, may hold values from -3 to 3
- pool_scale: float32 [2048], replicated, may hold values from 0.1 to 1.9
- gain_first: float32 [2048], replicated, may hold values from 0.1 to 1.9
- gain_mix: float32 [2048], replicated, may hold values from 0.1 to 1.9
- gain_second: float32 [2048], replicated, may hold values from 0.1 to 1.9
Outputs:
- result: bfloat16 [3072, 2048], P(('grp', 'fs')), parts along dimension 0
The draws below stay inside these ranges and needn't reach their ends.
There are 2 independent parts, one for each index of `grp`. The reference program is written for one: setup_inputs(seed, part) draws one part's arguments, and reference() takes and returns one part's arrays. A program takes and returns all parts, laid end to end along the dimension named above; an argument that names none is the same for every part. Nothing has to cross between parts.
All inputs are finite; a program needn't handle non-finite values.
Results may differ from the reference program's by a relative error of at most 0.018.
Values may be sent and summed in bfloat16 or wider, within the bound.
A program may use at most 64 MiB of HBM per device.

```python
import jax
import jax.numpy as jnp
from jax import lax

D = 2048
FF = 5120
TOK_DEV = 384
TOKENS = 1536
N_FS = 4
N_TP = 4


def level_of(stream_key, extent, split, least, high):
    level, own = 1.0, jax.random.fold_in(stream_key, 6)
    for dim, blocks in split:
        heights = jnp.exp(jax.random.uniform(jax.random.fold_in(own, dim), (blocks,), jnp.float32, least / len(split), high / len(split)))
        level = level * jnp.repeat(heights, extent[dim] // blocks).reshape([-1 if axis == dim else 1 for axis in range(len(extent))])
    return level


def normal_values(stream_key, dims, spread, bound, pieces=(), kind=jnp.bfloat16):
    loudness = level_of(stream_key, dims, pieces, -0.22, 0.18) if pieces else 1.0
    values = jax.random.normal(stream_key, dims, jnp.float32) * spread * loudness
    return jnp.minimum(jnp.maximum(values, -bound), bound).astype(kind)


def setup_inputs(seed: int = 0, part: int = 0) -> dict:
    splits = jax.random.split(jax.random.key(seed), 11)
    part_keys = jax.random.split(jax.random.fold_in(splits[10], part), 11)
    return {
        "tokens": normal_values(part_keys[0], (TOKENS, D), 0.5, 3.0, ((0, 4),)),
        "gate_weight": normal_values(splits[1], (D, FF), D ** -0.5, 0.125, ((0, 4), (1, 4))),
        "up_weight": normal_values(splits[2], (D, FF), D ** -0.5, 0.125, ((0, 4), (1, 4))),
        "down_weight": normal_values(splits[3], (FF, D), FF ** -0.5, 0.078125, ((0, 4), (1, 4))),
        "pool_weight": normal_values(splits[4], (D // 4, 4, D // 4), (D // 8) ** -0.5, 0.375, ((0, 4), (2, 4))),
        "pool_bias": normal_values(splits[5], (4, D // 4), 0.5, 3.0, (), jnp.float32),
        "pool_scale": jnp.clip(1.0 + 0.18 * jax.random.normal(splits[6], (D,), jnp.float32), 0.1, 1.9),
        "gain_first": jnp.clip(1.0 + 0.18 * jax.random.normal(splits[7], (D,), jnp.float32), 0.1, 1.9),
        "gain_mix": jnp.clip(1.0 + 0.18 * jax.random.normal(splits[8], (D,), jnp.float32), 0.1, 1.9),
        "gain_second": jnp.clip(1.0 + 0.18 * jax.random.normal(splits[9], (D,), jnp.float32), 0.1, 1.9),
    }


eps = 1e-06
pool_spans = (2, 4, 8, 16)

def rms_scale(values, gain_vec):
    fvalues = values.astype(jnp.float32)
    scaled = fvalues * lax.rsqrt(lax.optimization_barrier(jnp.mean(fvalues * fvalues, axis=-1, keepdims=True)) + eps)
    return (scaled * gain_vec).astype(jnp.bfloat16)

def ffn_hidden(normed, gate_weight, up_weight):
    gate_proj = jnp.dot(normed, gate_weight, preferred_element_type=jnp.float32)
    up_proj = jnp.dot(normed, up_weight, preferred_element_type=jnp.float32)
    return (jax.nn.silu(gate_proj) * up_proj).astype(jnp.bfloat16)

def down_sum(hidden, down_weight):
    block_width = FF // N_TP
    summed = jnp.zeros((hidden.shape[0], D), jnp.float32)
    for block_index in range(N_TP):
        lower_row = block_index * block_width
        partial_sum = jnp.dot(hidden[:, lower_row:lower_row + block_width], down_weight[lower_row:lower_row + block_width], preferred_element_type=jnp.float32)
        rounded = lax.optimization_barrier(partial_sum.astype(jnp.bfloat16))
        summed = summed + rounded.astype(jnp.float32)
    return summed

def pool_mix(normed, pool_weight, pool_bias, pool_scale):
    seq_len = normed.shape[0]
    group_width = D // 4
    grouped = normed.astype(jnp.float32).reshape(seq_len, 4, group_width)
    running = jnp.concatenate([jnp.zeros((1, 4, group_width), jnp.float32), jnp.cumsum(grouped, axis=0)], axis=0)
    position = jnp.arange(seq_len, dtype=jnp.int32)[:, None]
    spans = jnp.array(pool_spans, dtype=jnp.int32)[None, :]
    low_edge = jnp.clip(position - spans // 2, 0, seq_len)
    high_edge = jnp.clip(position - spans // 2 + spans, 0, seq_len)
    group_index = jnp.arange(4, dtype=jnp.int32)[None, :]
    counts = (high_edge - low_edge).astype(jnp.float32)[:, :, None]
    window_mean = (running[high_edge, group_index] - running[low_edge, group_index]) / counts
    deviation = (window_mean - grouped).astype(jnp.bfloat16)
    outputs = []
    for group_number in range(4):
        mapped = jnp.dot(deviation[:, group_number, :], pool_weight[:, group_number, :], preferred_element_type=jnp.float32)
        outputs.append(mapped + pool_bias[group_number])
    return jnp.concatenate(outputs, axis=-1) * pool_scale

def reference(tokens, gate_weight, up_weight, down_weight, pool_weight, pool_bias, pool_scale, gain_first, gain_mix, gain_second):

    def one_sequence(seq_rows):
        first_normed = rms_scale(seq_rows, gain_first)
        first_hidden = ffn_hidden(first_normed, gate_weight, up_weight)
        after_first = (seq_rows.astype(jnp.float32) + 0.5 * down_sum(first_hidden, down_weight)).astype(jnp.bfloat16)
        mix_normed = rms_scale(after_first, gain_mix)
        mixed = pool_mix(mix_normed, pool_weight, pool_bias, pool_scale)
        after_mix = (after_first.astype(jnp.float32) + mixed).astype(jnp.bfloat16)
        second_normed = rms_scale(after_mix, gain_second)
        second_hidden = ffn_hidden(second_normed, gate_weight, up_weight)
        return (after_mix.astype(jnp.float32) + 0.5 * down_sum(second_hidden, down_weight)).astype(jnp.bfloat16)
    sequences = tokens.reshape(N_FS, TOK_DEV, D)
    return lax.map(one_sequence, sequences).reshape(TOKENS, D)
```

```python
import functools

import jax
import jax.numpy as jnp
from jax import lax
from jax.experimental import pallas as pl
from jax.experimental.pallas import tpu as pltpu
from jax.sharding import PartitionSpec as P

eps = 1e-06
pool_spans = (2, 4, 8, 16)
pad_width = 8
MESH = pl.DeviceIdType.MESH


def rms_scale(values, gain_vec):
    fvalues = values.astype(jnp.float32)
    scaled = fvalues * lax.rsqrt(jnp.mean(fvalues * fvalues, axis=-1, keepdims=True) + eps)
    return (scaled * gain_vec).astype(jnp.bfloat16)


def ffn_hidden(normed, gate_full, up_full):
    gate_proj = jnp.dot(normed, gate_full, preferred_element_type=jnp.float32)
    up_proj = jnp.dot(normed, up_full, preferred_element_type=jnp.float32)
    return (jax.nn.silu(gate_proj) * up_proj).astype(jnp.bfloat16)


def pool_block(padded, offset, seq_len, pool_full, pool_bias, pool_scale):
    n_tokens = padded.shape[0] - 2 * pad_width
    group_width = pool_full.shape[0]
    position = offset + lax.iota(jnp.int32, n_tokens)
    column_pos = offset - pad_width + lax.iota(jnp.int32, padded.shape[0])
    center = padded[pad_width : pad_width + n_tokens].astype(jnp.float32)
    outputs = []
    for group_number, window_span in enumerate(pool_spans):
        low_edge = jnp.clip(position - window_span // 2, 0, seq_len)
        high_edge = jnp.clip(position - window_span // 2 + window_span, 0, seq_len)
        band_mask = (
            (column_pos[None, :] >= low_edge[:, None]) & (column_pos[None, :] < high_edge[:, None])
        ).astype(jnp.bfloat16)
        lower_col = group_number * group_width
        columns = padded[:, lower_col : lower_col + group_width]
        window_sum = jnp.dot(band_mask, columns, preferred_element_type=jnp.float32)
        window_mean = window_sum / (high_edge - low_edge).astype(jnp.float32)[:, None]
        deviation = (window_mean - center[:, lower_col : lower_col + group_width]).astype(
            jnp.bfloat16
        )
        mapped = jnp.dot(
            deviation, pool_full[:, group_number, :], preferred_element_type=jnp.float32
        )
        outputs.append(mapped + pool_bias[group_number])
    return jnp.concatenate(outputs, axis=-1) * pool_scale


def shards(
    tokens,
    gate_weight,
    up_weight,
    down_weight,
    pool_weight,
    pool_bias,
    pool_scale,
    gain_first,
    gain_mix,
    gain_second,
):
    gate_full, up_full, pool_half = (
        lax.all_gather(gate_weight, "fs", axis=0, tiled=True),
        lax.all_gather(up_weight, "fs", axis=0, tiled=True),
        lax.all_gather(pool_weight, "fs", axis=0, tiled=True),
    )
    down_full = lax.all_gather(down_weight, "fs", axis=1, tiled=True)
    pool_full = lax.all_gather(pool_half, "tp", axis=2, tiled=True)
    seq_len = tokens.shape[0]
    first_normed = rms_scale(tokens, gain_first)
    first_hidden = ffn_hidden(first_normed, gate_full, up_full)
    second_gate, second_up, second_down = (gate_full, up_full, down_full)
    first_branch = lax.psum(
        jnp.dot(first_hidden, down_full, preferred_element_type=jnp.float32).astype(jnp.bfloat16),
        "tp",
    ).astype(jnp.float32)
    after_first = (tokens.astype(jnp.float32) + 0.5 * first_branch).astype(jnp.bfloat16)
    mix_normed = rms_scale(after_first, gain_mix)
    padded = jnp.pad(mix_normed, ((pad_width, pad_width), (0, 0)))
    mixed = pool_block(padded, 0, seq_len, pool_full, pool_bias, pool_scale)
    after_mix = (after_first.astype(jnp.float32) + mixed).astype(jnp.bfloat16)
    second_normed = rms_scale(after_mix, gain_second)
    second_hidden = ffn_hidden(second_normed, second_gate, second_up)
    second_branch = lax.psum(
        jnp.dot(second_hidden, second_down, preferred_element_type=jnp.float32).astype(
            jnp.bfloat16
        ),
        "tp",
    ).astype(jnp.float32)
    return (after_mix.astype(jnp.float32) + 0.5 * second_branch).astype(jnp.bfloat16)


def fused_kernel(
    sizes, tok_ref, gate_ref, up_ref, down_ref, pool_ref, bias_ref, scale_ref, gain1_ref, gainm_ref, gain2_ref,
    out_ref,
    gu_full, down_full, pool_full, acc, normed, hidden, amix, res, part, rbuf, xs, xr,
    zsend, zleft, zrecv, ysend, yrecv, tsend, trecv, lsem, csend, crecv, xsend, xrecv, fsend, frecv, osem,
):
    n, n_tp = sizes
    g, z, t = lax.axis_index("grp"), lax.axis_index("fs"), lax.axis_index("tp")
    core = lax.rem(t, 2)
    y_peer, right, left = {"grp": 1 - g}, {"fs": z + 1}, {"fs": z - 1}
    mate, x_peer = {"tp": t + 1 - 2 * core}, {"tp": lax.rem(t + 2, n_tp)}
    n_rows, width = tok_ref.shape
    d_loc, f_loc = gate_ref.shape
    groups, pool_rows, pool_cols = pool_ref.shape
    half_rows = n_rows // 2
    f32 = jnp.float32

    def remote(src, dst, s_sem, r_sem, dev):
        return pltpu.make_async_remote_copy(
            src_ref=src, dst_ref=dst, send_sem=s_sem, recv_sem=r_sem, device_id=dev, device_id_type=MESH
        )

    barrier = pltpu.get_barrier_semaphore()

    def greet(dev):
        pl.semaphore_signal(barrier, inc=1, device_id=dev, device_id_type=MESH)

    greet(y_peer)
    for off in range(1, n_tp):
        greet({"tp": lax.rem(t + off, n_tp)})

    @pl.when(z > 0)
    def _():
        greet(left)

    @pl.when(z < n - 1)
    def _():
        greet(right)

    pl.semaphore_wait(barrier, n_tp + jnp.minimum(z, 1) + jnp.minimum(n - 1 - z, 1))

    pieces = [("pool", 0, 1)] + [(name, c, 2) for name in ("gate", "up", "down") for c in range(2)]
    n_pieces = len(pieces)

    def rows_of(name, half, c, count):
        total = {"pool": pool_rows, "gate": d_loc, "up": d_loc, "down": f_loc}[name]
        size = total // (2 * count)
        return half * (total // 2) + c * size, size, total

    def region(name, s, half, c, count):
        start, size, total = rows_of(name, half, c, count)
        if name == "down":
            return down_full.at[s, pl.ds(pl.multiple_of(start, 16), size), :]
        rows = pl.ds(pl.multiple_of(s * total + start, 16), size)
        if name == "pool":
            return pool_full.at[:, rows, pl.ds(pl.multiple_of(t * pool_cols, 128), pool_cols)]
        return gu_full.at[0 if name == "gate" else 1, rows, :]

    def source(name, half, c, count):
        start, size, _ = rows_of(name, half, c, count)
        rows = pl.ds(pl.multiple_of(start, 16), size)
        if name == "pool":
            return pool_ref.at[:, rows, :]
        return {"gate": gate_ref, "up": up_ref, "down": down_ref}[name].at[rows, :]

    def own_right(k):
        name, c, count = pieces[k]
        return remote(source(name, g, c, count), region(name, z, g, c, count), zsend.at[z, k], zrecv.at[z, k], right)

    def own_left(k):
        name, c, count = pieces[k]
        return remote(source(name, g, c, count), region(name, z, g, c, count), zleft.at[k], zrecv.at[z, k], left)

    def pass_on(k, s, dev):
        name, c, count = pieces[k]
        there = region(name, s, g, c, count)
        return remote(there, there, zsend.at[s, k], zrecv.at[s, k], dev)

    def share(k, s, half):
        name, c, count = pieces[k]
        there = region(name, s, half, c, count)
        return remote(there, there, ysend.at[s, k], yrecv.at[s, k], y_peer)

    for k in range(n_pieces):

        @pl.when(z < n - 1)
        def _():
            own_right(k).start()

        @pl.when(z > 0)
        def _():
            own_left(k).start()

    own_rows = pl.ds(pl.multiple_of(z * d_loc, 128), d_loc)
    own_pool = pool_full.at[
        :, pl.ds(pl.multiple_of(z * pool_rows, 16), pool_rows), pl.ds(pl.multiple_of(t * pool_cols, 128), pool_cols)
    ]
    local = [
        pltpu.make_async_copy(pool_ref, own_pool, lsem.at[0]),
        pltpu.make_async_copy(gate_ref, gu_full.at[0, own_rows, :], lsem.at[1]),
        pltpu.make_async_copy(up_ref, gu_full.at[1, own_rows, :], lsem.at[2]),
        pltpu.make_async_copy(down_ref, down_full.at[z], lsem.at[3]),
    ]
    for copy in local:
        copy.start()

    def norm_rows(src, gain):
        @pl.loop(0, n_rows // 32)
        def _(r):
            rows = pl.ds(pl.multiple_of(r * 32, 32), 32)
            values = src[rows, :].astype(f32)
            scaled = values * lax.rsqrt(jnp.mean(values * values, axis=-1, keepdims=True) + eps)
            normed[rows, :] = (scaled * gain[...]).astype(jnp.bfloat16)

    tile = 256

    def add_shard(w, s):
        k_cols = pl.ds(pl.multiple_of(s * d_loc, 128), d_loc)

        @pl.loop(0, f_loc // tile)
        def _(i):
            cols = pl.ds(pl.multiple_of(i * tile, tile), tile)
            acc[w, :, cols] += jnp.dot(normed[:, k_cols], gu_full[w, k_cols, cols], preferred_element_type=f32)

    def pool_copy(off, s, sender):
        cols = pl.ds(pl.multiple_of(sender * pool_cols, 128), pool_cols)
        there = pool_full.at[:, pl.ds(pl.multiple_of(s * pool_rows, 16), pool_rows), cols]
        return remote(there, there, tsend.at[off - 1, s], trecv.at[off - 1, s], {"tp": lax.rem(t + off, n_tp)})

    def spread_pool(s):
        for off in range(1, n_tp):
            pool_copy(off, s, t).start()

    norm_rows(tok_ref, gain1_ref)
    acc[...] = jnp.zeros_like(acc)
    for copy in local:
        copy.wait()
    spread_pool(z)

    @pl.loop(0, 2)
    def _(w):
        add_shard(w, z)

    def both_sides(d, act):
        @pl.when(z >= d)
        def _():
            act(z - d, z < n - 1, right)

        @pl.when(z + d < n)
        def _():
            act(z + d, z > 0, left)

    def relay(name, d):
        for k in range(n_pieces):
            if pieces[k][0] != name:
                continue

            def act(s, more, dev):
                pass_on(k, s, dev).wait_recv()

                @pl.when(more)
                def _():
                    pass_on(k, s, dev).start()

                share(k, s, g).start()

            both_sides(d, act)

    def settle(name, s):
        for k in range(n_pieces):
            if pieces[k][0] == name:
                share(k, s, 1 - g).wait_recv()

    def settle_pool(s, *_):
        settle("pool", s)
        spread_pool(s)

    def settle_gate(s, *_):
        settle("gate", s)
        add_shard(0, s)

    def settle_up(s, *_):
        settle("up", s)
        add_shard(1, s)

    @pl.loop(1, n)
    def _(d):
        relay("pool", d)
        relay("gate", d)
        both_sides(d, settle_pool)
        relay("up", d)
        both_sides(d, settle_gate)
        relay("down", d)
        both_sides(d, settle_up)

    def activate(gate_proj, up_proj):
        return (gate_proj / (1.0 + jnp.exp(-gate_proj)) * up_proj).astype(jnp.bfloat16)

    @pl.loop(0, f_loc // tile)
    def _(i):
        cols = pl.ds(pl.multiple_of(i * tile, tile), tile)
        hidden[:, cols] = activate(acc[0, :, cols], acc[1, :, cols])

    turn = 1 - 2 * ((2 * z) // n)
    mine = pl.ds(pl.multiple_of(core * half_rows, 16), half_rows)
    other = pl.ds(pl.multiple_of((1 - core) * half_rows, 16), half_rows)

    def branch_sum(phase, base):
        def block(j):
            return lax.rem(z + turn * j + n, n)

        def pair_copy(j):
            return remote(part.at[phase, j, other, :], rbuf.at[phase, j], csend.at[phase, j], crecv.at[phase, j], mate)

        def x_copy(j):
            return remote(xs.at[phase, j], xr.at[phase, j], xsend.at[phase, j], xrecv.at[phase, j], x_peer)

        def final_copy(j, rows):
            there = res.at[phase, rows, pl.ds(pl.multiple_of(block(j) * d_loc, 128), d_loc)]
            return remote(there, there, fsend.at[phase, j], frecv.at[phase, j], mate)

        def multiply(j):
            s = block(j)
            if phase == 0 and j > 0:
                settle("down", s)

            @pl.loop(0, d_loc // tile)
            def _(i):
                cols = pl.ds(pl.multiple_of(i * tile, tile), tile)
                part[phase, j, :, cols] = jnp.dot(
                    hidden[...], down_full[s, :, cols], preferred_element_type=f32
                ).astype(jnp.bfloat16)

            pair_copy(j).start()

        def add_pair(j):
            pair_copy(j).wait_recv()
            xs[phase, j] = (part[phase, j, mine, :].astype(f32) + rbuf[phase, j].astype(f32)).astype(jnp.bfloat16)
            x_copy(j).start()

        def finish(j):
            x_copy(j).wait_recv()
            total = xs[phase, j].astype(f32) + xr[phase, j].astype(f32)
            cols = pl.ds(pl.multiple_of(block(j) * d_loc, 128), d_loc)
            res[phase, mine, cols] = (base[mine, cols].astype(f32) + 0.5 * total).astype(jnp.bfloat16)
            final_copy(j, mine).start()

        for j in range(n + 1):
            if j < n:
                multiply(j)
            if j > 0:
                add_pair(j - 1)
        for j in range(n):
            finish(j)
        for j in range(n):
            final_copy(j, other).wait_recv()

        def drain():
            for j in range(n):
                pair_copy(j).wait_send()
                x_copy(j).wait_send()
                final_copy(j, mine).wait_send()

        return drain

    drain_first = branch_sum(0, tok_ref)

    norm_rows(res.at[0], gainm_ref)
    for off in range(1, n_tp):
        for s in range(n):
            pool_copy(off, s, lax.rem(t - off + n_tp, n_tp)).wait_recv()
    group_width = width // groups
    row_id = lax.broadcasted_iota(jnp.int32, (n_rows, n_rows), 0)
    col_id = lax.broadcasted_iota(jnp.int32, (n_rows, n_rows), 1)
    position = lax.broadcasted_iota(jnp.int32, (n_rows, 1), 0)
    for k, span in enumerate(pool_spans):
        low = row_id - span // 2
        band = jnp.where((col_id >= low) & (col_id < low + span), 1.0, 0.0).astype(jnp.bfloat16)
        first = jnp.maximum(position - span // 2, 0)
        last = jnp.minimum(position - span // 2 + span, n_rows)
        inverse = 1.0 / (last - first).astype(f32)
        cols = pl.ds(k * group_width, group_width)
        mean = jnp.dot(band, normed[:, cols], preferred_element_type=f32) * inverse
        deviation = (mean - normed[:, cols].astype(f32)).astype(jnp.bfloat16)
        mapped = jnp.dot(deviation, pool_full[k], preferred_element_type=f32) + bias_ref[pl.ds(k, 1), :]
        amix[:, cols] = (res[0, :, cols].astype(f32) + mapped * scale_ref[:, cols]).astype(jnp.bfloat16)

    norm_rows(amix, gain2_ref)

    @pl.loop(0, f_loc // tile)
    def _(i):
        cols = pl.ds(pl.multiple_of(i * tile, tile), tile)
        gate_proj = jnp.dot(normed[...], gu_full[0, :, cols], preferred_element_type=f32)
        up_proj = jnp.dot(normed[...], gu_full[1, :, cols], preferred_element_type=f32)
        hidden[:, cols] = activate(gate_proj, up_proj)

    drain_second = branch_sum(1, amix)
    out_copy = pltpu.make_async_copy(res.at[1], out_ref, osem)
    out_copy.start()

    for k in range(n_pieces):

        @pl.when(z < n - 1)
        def _():
            own_right(k).wait_send()

        @pl.when(z > 0)
        def _():
            own_left(k).wait_send()

    @pl.loop(1, n)
    def _(d):
        for k in range(n_pieces):

            def act(s, more, dev):
                @pl.when(more)
                def _():
                    pass_on(k, s, dev).wait_send()

                share(k, s, g).wait_send()

            both_sides(d, act)

    @pl.loop(0, n)
    def _(s):
        for off in range(1, n_tp):
            pool_copy(off, s, t).wait_send()

    drain_first()
    drain_second()
    out_copy.wait()


def fused_shards(
    n, n_tp, tokens, gate_weight, up_weight, down_weight, pool_weight, pool_bias, pool_scale,
    gain_first, gain_mix, gain_second,
):
    n_rows, width = tokens.shape
    d_loc, f_loc = gate_weight.shape
    groups = pool_weight.shape[1]
    pool = jnp.swapaxes(pool_weight, 0, 1)
    bf16, dma, vmem = jnp.bfloat16, pltpu.SemaphoreType.DMA, pltpu.VMEM
    in_vmem, anywhere = pl.BlockSpec(memory_space=pltpu.VMEM), pl.BlockSpec(memory_space=pl.ANY)
    half = n_rows // 2
    return pl.pallas_call(
        functools.partial(fused_kernel, (n, n_tp)),
        out_shape=jax.ShapeDtypeStruct((n_rows, width), bf16),
        in_specs=[in_vmem] + [anywhere] * 4 + [in_vmem] * 5,
        out_specs=anywhere,
        scratch_shapes=[
            vmem((2, n * d_loc, f_loc), bf16),
            vmem((n, f_loc, d_loc), bf16),
            vmem((groups, n * pool.shape[1], n_tp * pool.shape[2]), bf16),
            vmem((2, n_rows, f_loc), jnp.float32),
            vmem((n_rows, width), bf16),
            vmem((n_rows, f_loc), bf16),
            vmem((n_rows, width), bf16),
            vmem((2, n_rows, width), bf16),
            vmem((2, n, n_rows, d_loc), bf16),
            vmem((2, n, half, d_loc), bf16),
            vmem((2, n, half, d_loc), bf16),
            vmem((2, n, half, d_loc), bf16),
            dma((n, 7)), dma((7,)), dma((n, 7)), dma((n, 7)), dma((n, 7)),
            dma((n_tp - 1, n)), dma((n_tp - 1, n)), dma((4,)),
            dma((2, n)), dma((2, n)), dma((2, n)), dma((2, n)), dma((2, n)), dma((2, n)), dma,
        ],
        compiler_params=pltpu.CompilerParams(
            collective_id=0, has_side_effects=True, vmem_limit_bytes=60 * 1024 * 1024
        ),
    )(
        tokens, gate_weight, up_weight, down_weight, pool, pool_bias, pool_scale.reshape(1, width),
        gain_first.reshape(1, width), gain_mix.reshape(1, width), gain_second.reshape(1, width),
    )


def layer(n_grp, n, n_tp, *args):
    n_rows, width = args[0].shape
    d_loc, f_loc = args[1].shape
    pool_rows, _, pool_cols = args[4].shape
    fits = n_grp == 2 and n_tp == 4 and n % 2 == 0 and n <= 4 and n_rows % 64 == 0
    fits = fits and d_loc % 256 == 0 and f_loc % 256 == 0 and pool_rows % 32 == 0 and pool_cols % 128 == 0
    return fused_shards(n, n_tp, *args) if fits else shards(*args)


def solution(mesh):
    return jax.shard_map(
        functools.partial(layer, mesh.shape["grp"], mesh.shape["fs"], mesh.shape["tp"]),
        mesh=mesh,
        in_specs=(
            P(("grp", "fs"), None),
            P("fs", "tp"),
            P("fs", "tp"),
            P("tp", "fs"),
            P("fs", None, "tp"),
            P(),
            P(),
            P(),
            P(),
            P(),
        ),
        out_specs=P(("grp", "fs"), None),
        check_vma=False,
    )
```

```python
import functools

import jax
import jax.numpy as jnp
from jax import lax
from jax.experimental import pallas as pl
from jax.experimental.pallas import tpu as pltpu
from jax.sharding import PartitionSpec as P

eps = 1e-06
pool_spans = (2, 4, 8, 16)
pad_width = 8
MESH = pl.DeviceIdType.MESH


def rms_scale(values, gain_vec):
    fvalues = values.astype(jnp.float32)
    scaled = fvalues * lax.rsqrt(jnp.mean(fvalues * fvalues, axis=-1, keepdims=True) + eps)
    return (scaled * gain_vec).astype(jnp.bfloat16)


def ffn_hidden(normed, gate_full, up_full):
    gate_proj = jnp.dot(normed, gate_full, preferred_element_type=jnp.float32)
    up_proj = jnp.dot(normed, up_full, preferred_element_type=jnp.float32)
    return (jax.nn.silu(gate_proj) * up_proj).astype(jnp.bfloat16)


def pool_block(padded, offset, seq_len, pool_full, pool_bias, pool_scale):
    n_tokens = padded.shape[0] - 2 * pad_width
    group_width = pool_full.shape[0]
    position = offset + lax.iota(jnp.int32, n_tokens)
    column_pos = offset - pad_width + lax.iota(jnp.int32, padded.shape[0])
    center = padded[pad_width : pad_width + n_tokens].astype(jnp.float32)
    outputs = []
    for group_number, window_span in enumerate(pool_spans):
        low_edge = jnp.clip(position - window_span // 2, 0, seq_len)
        high_edge = jnp.clip(position - window_span // 2 + window_span, 0, seq_len)
        band_mask = (
            (column_pos[None, :] >= low_edge[:, None]) & (column_pos[None, :] < high_edge[:, None])
        ).astype(jnp.bfloat16)
        lower_col = group_number * group_width
        columns = padded[:, lower_col : lower_col + group_width]
        window_sum = jnp.dot(band_mask, columns, preferred_element_type=jnp.float32)
        window_mean = window_sum / (high_edge - low_edge).astype(jnp.float32)[:, None]
        deviation = (window_mean - center[:, lower_col : lower_col + group_width]).astype(
            jnp.bfloat16
        )
        mapped = jnp.dot(
            deviation, pool_full[:, group_number, :], preferred_element_type=jnp.float32
        )
        outputs.append(mapped + pool_bias[group_number])
    return jnp.concatenate(outputs, axis=-1) * pool_scale


def shards(
    tokens,
    gate_weight,
    up_weight,
    down_weight,
    pool_weight,
    pool_bias,
    pool_scale,
    gain_first,
    gain_mix,
    gain_second,
):
    gate_full, up_full, pool_half = (
        lax.all_gather(gate_weight, "fs", axis=0, tiled=True),
        lax.all_gather(up_weight, "fs", axis=0, tiled=True),
        lax.all_gather(pool_weight, "fs", axis=0, tiled=True),
    )
    down_full = lax.all_gather(down_weight, "fs", axis=1, tiled=True)
    pool_full = lax.all_gather(pool_half, "tp", axis=2, tiled=True)
    seq_len = tokens.shape[0]
    first_normed = rms_scale(tokens, gain_first)
    first_hidden = ffn_hidden(first_normed, gate_full, up_full)
    second_gate, second_up, second_down = (gate_full, up_full, down_full)
    first_branch = lax.psum(
        jnp.dot(first_hidden, down_full, preferred_element_type=jnp.float32).astype(jnp.bfloat16),
        "tp",
    ).astype(jnp.float32)
    after_first = (tokens.astype(jnp.float32) + 0.5 * first_branch).astype(jnp.bfloat16)
    mix_normed = rms_scale(after_first, gain_mix)
    padded = jnp.pad(mix_normed, ((pad_width, pad_width), (0, 0)))
    mixed = pool_block(padded, 0, seq_len, pool_full, pool_bias, pool_scale)
    after_mix = (after_first.astype(jnp.float32) + mixed).astype(jnp.bfloat16)
    second_normed = rms_scale(after_mix, gain_second)
    second_hidden = ffn_hidden(second_normed, second_gate, second_up)
    second_branch = lax.psum(
        jnp.dot(second_hidden, second_down, preferred_element_type=jnp.float32).astype(
            jnp.bfloat16
        ),
        "tp",
    ).astype(jnp.float32)
    return (after_mix.astype(jnp.float32) + 0.5 * second_branch).astype(jnp.bfloat16)


def fused_kernel(
    sizes, tok_ref, gate_ref, up_ref, down_ref, pool_ref, bias_ref, scale_ref, gain1_ref, gainm_ref, gain2_ref,
    out_ref,
    gu_full, down_full, pool_full, acc, normed, hidden, amix, res, part, rbuf, xs, xr,
    zsend, zleft, zrecv, ysend, yrecv, tsend, trecv, lsem, csend, crecv, xsend, xrecv, fsend, frecv, osem,
):
    n, n_tp = sizes
    g, z, t = lax.axis_index("grp"), lax.axis_index("fs"), lax.axis_index("tp")
    core = lax.rem(t, 2)
    y_peer, right, left = {"grp": 1 - g}, {"fs": z + 1}, {"fs": z - 1}
    mate, x_peer = {"tp": t + 1 - 2 * core}, {"tp": lax.rem(t + 2, n_tp)}
    n_rows, width = tok_ref.shape
    d_loc, f_loc = gate_ref.shape
    groups, pool_rows, pool_cols = pool_ref.shape
    half_rows = n_rows // 2
    block_cols = d_loc // 2
    f32 = jnp.float32

    def remote(src, dst, s_sem, r_sem, dev):
        return pltpu.make_async_remote_copy(
            src_ref=src, dst_ref=dst, send_sem=s_sem, recv_sem=r_sem, device_id=dev, device_id_type=MESH
        )

    barrier = pltpu.get_barrier_semaphore()

    def greet(dev):
        pl.semaphore_signal(barrier, inc=1, device_id=dev, device_id_type=MESH)

    greet(y_peer)
    for off in range(1, n_tp):
        greet({"tp": lax.rem(t + off, n_tp)})

    @pl.when(z > 0)
    def _():
        greet(left)

    @pl.when(z < n - 1)
    def _():
        greet(right)

    pl.semaphore_wait(barrier, n_tp + jnp.minimum(z, 1) + jnp.minimum(n - 1 - z, 1))

    pieces = [("pool", 0, 1)] + [(name, c, 4) for name in ("gate", "up", "down") for c in range(4)]
    n_pieces = len(pieces)

    def rows_of(name, half, c, count):
        if name == "down":
            return c * (f_loc // count), f_loc // count, f_loc
        total = {"pool": pool_rows, "gate": d_loc, "up": d_loc}[name]
        size = total // (2 * count)
        return half * (total // 2) + c * size, size, total

    def region(name, s, half, c, count):
        start, size, total = rows_of(name, half, c, count)
        if name == "down":
            return down_full.at[s, half, pl.ds(start, size), :]
        rows = pl.ds(pl.multiple_of(s * total + start, 16), size)
        if name == "pool":
            return pool_full.at[:, rows, pl.ds(pl.multiple_of(t * pool_cols, 128), pool_cols)]
        return gu_full.at[0 if name == "gate" else 1, rows, :]

    def source(name, half, c, count):
        start, size, _ = rows_of(name, half, c, count)
        if name == "down":
            return down_ref.at[pl.ds(start, size), pl.ds(pl.multiple_of(half * block_cols, 128), block_cols)]
        rows = pl.ds(pl.multiple_of(start, 16), size)
        if name == "pool":
            return pool_ref.at[:, rows, :]
        return {"gate": gate_ref, "up": up_ref}[name].at[rows, :]

    def own_right(k):
        name, c, count = pieces[k]
        return remote(source(name, g, c, count), region(name, z, g, c, count), zsend.at[z, k], zrecv.at[z, k], right)

    def own_left(k):
        name, c, count = pieces[k]
        return remote(source(name, g, c, count), region(name, z, g, c, count), zleft.at[k], zrecv.at[z, k], left)

    def pass_on(k, s, dev):
        name, c, count = pieces[k]
        there = region(name, s, g, c, count)
        return remote(there, there, zsend.at[s, k], zrecv.at[s, k], dev)

    def share(k, s, half):
        name, c, count = pieces[k]
        there = region(name, s, half, c, count)
        return remote(there, there, ysend.at[s, k], yrecv.at[s, k], y_peer)

    for k in range(n_pieces):

        @pl.when(z < n - 1)
        def _():
            own_right(k).start()

        @pl.when(z > 0)
        def _():
            own_left(k).start()

    own_rows = pl.ds(pl.multiple_of(z * d_loc, 128), d_loc)
    own_pool = pool_full.at[
        :, pl.ds(pl.multiple_of(z * pool_rows, 16), pool_rows), pl.ds(pl.multiple_of(t * pool_cols, 128), pool_cols)
    ]
    local = [
        pltpu.make_async_copy(pool_ref, own_pool, lsem.at[0]),
        pltpu.make_async_copy(gate_ref, gu_full.at[0, own_rows, :], lsem.at[1]),
        pltpu.make_async_copy(up_ref, gu_full.at[1, own_rows, :], lsem.at[2]),
        pltpu.make_async_copy(down_ref.at[:, pl.ds(0, block_cols)], down_full.at[z, 0], lsem.at[3]),
        pltpu.make_async_copy(down_ref.at[:, pl.ds(block_cols, block_cols)], down_full.at[z, 1], lsem.at[4]),
    ]
    for copy in local:
        copy.start()

    def norm_rows(src, gain):
        @pl.loop(0, n_rows // 32)
        def _(r):
            rows = pl.ds(pl.multiple_of(r * 32, 32), 32)
            values = src[rows, :].astype(f32)
            scaled = values * lax.rsqrt(jnp.mean(values * values, axis=-1, keepdims=True) + eps)
            normed[rows, :] = (scaled * gain[...]).astype(jnp.bfloat16)

    tile = 256

    def add_shard(w, s):
        k_cols = pl.ds(pl.multiple_of(s * d_loc, 128), d_loc)

        @pl.loop(0, f_loc // tile)
        def _(i):
            cols = pl.ds(pl.multiple_of(i * tile, tile), tile)
            acc[w, :, cols] += jnp.dot(normed[:, k_cols], gu_full[w, k_cols, cols], preferred_element_type=f32)

    def pool_copy(off, s, sender):
        cols = pl.ds(pl.multiple_of(sender * pool_cols, 128), pool_cols)
        there = pool_full.at[:, pl.ds(pl.multiple_of(s * pool_rows, 16), pool_rows), cols]
        return remote(there, there, tsend.at[off - 1, s], trecv.at[off - 1, s], {"tp": lax.rem(t + off, n_tp)})

    def spread_pool(s):
        for off in range(1, n_tp):
            pool_copy(off, s, t).start()

    norm_rows(tok_ref, gain1_ref)
    acc[...] = jnp.zeros_like(acc)
    for copy in local:
        copy.wait()
    spread_pool(z)

    @pl.loop(0, 2)
    def _(w):
        add_shard(w, z)

    def both_sides(d, act):
        @pl.when(z >= d)
        def _():
            act(z - d, z < n - 1, right)

        @pl.when(z + d < n)
        def _():
            act(z + d, z > 0, left)

    def relay(name, d, only=None):
        for k in range(n_pieces):
            if pieces[k][0] != name or only not in (None, pieces[k][1]):
                continue

            def act(s, more, dev):
                pass_on(k, s, dev).wait_recv()

                @pl.when(more)
                def _():
                    pass_on(k, s, dev).start()

                share(k, s, g).start()

            both_sides(d, act)

    def settle(name, s):
        for k in range(n_pieces):
            if pieces[k][0] == name:
                share(k, s, 1 - g).wait_recv()

    def settle_pool(s, *_):
        settle("pool", s)
        spread_pool(s)

    def settle_gate(s, *_):
        settle("gate", s)
        add_shard(0, s)

    def settle_up(s, *_):
        settle("up", s)
        add_shard(1, s)

    @pl.loop(1, n - 1)
    def _(d):
        relay("pool", d)
        relay("gate", d)
        both_sides(d, settle_pool)
        relay("up", d)
        both_sides(d, settle_gate)
        relay("down", d)
        both_sides(d, settle_up)

    relay("pool", n - 1)
    relay("gate", n - 1)
    both_sides(n - 1, settle_pool)
    relay("up", n - 1)
    both_sides(n - 1, settle_gate)
    relay("down", n - 1, 0)
    both_sides(n - 1, settle_up)
    relay("down", n - 1, 1)

    def activate(gate_proj, up_proj):
        return (gate_proj / (1.0 + jnp.exp(-gate_proj)) * up_proj).astype(jnp.bfloat16)

    @pl.loop(0, f_loc // tile)
    def _(i):
        cols = pl.ds(pl.multiple_of(i * tile, tile), tile)
        hidden[:, cols] = activate(acc[0, :, cols], acc[1, :, cols])

    turn = 1 - 2 * ((2 * z) // n)
    mine = pl.ds(pl.multiple_of(core * half_rows, 16), half_rows)
    other = pl.ds(pl.multiple_of((1 - core) * half_rows, 16), half_rows)

    n_blocks = 2 * n

    def branch_sum(phase, base):
        def place(j):
            return lax.rem(z + turn * (j // 2) + n, n), g if j % 2 == 0 else 1 - g

        def columns(j):
            s, half = place(j)
            return pl.ds(pl.multiple_of(s * d_loc + half * block_cols, 128), block_cols)

        def pair_copy(j):
            return remote(part.at[phase, j, other, :], rbuf.at[phase, j], csend.at[phase, j], crecv.at[phase, j], mate)

        def x_copy(j):
            return remote(xs.at[phase, j], xr.at[phase, j], xsend.at[phase, j], xrecv.at[phase, j], x_peer)

        def final_copy(j, rows):
            there = res.at[phase, rows, columns(j)]
            return remote(there, there, fsend.at[phase, j], frecv.at[phase, j], mate)

        def multiply(j):
            s, half = place(j)
            if phase == 0 and j in (2, 3):
                relay("down", n - 1, j)
            if phase == 0 and j >= 2 and j % 2 == 1:
                settle("down", s)
            part[phase, j] = jnp.dot(
                hidden[...], down_full[s, half], preferred_element_type=f32
            ).astype(jnp.bfloat16)
            pair_copy(j).start()

        def add_pair(j):
            pair_copy(j).wait_recv()
            xs[phase, j] = (part[phase, j, mine, :].astype(f32) + rbuf[phase, j].astype(f32)).astype(jnp.bfloat16)
            x_copy(j).start()

        def finish(j):
            x_copy(j).wait_recv()
            total = xs[phase, j].astype(f32) + xr[phase, j].astype(f32)
            cols = columns(j)
            res[phase, mine, cols] = (base[mine, cols].astype(f32) + 0.5 * total).astype(jnp.bfloat16)
            final_copy(j, mine).start()

        early = n_blocks // 2 if phase == 0 else 0
        for j in range(n_blocks + 1):
            if j == n_blocks - 1:
                for done in range(early):
                    finish(done)
            if j < n_blocks:
                multiply(j)
            if j > 0:
                add_pair(j - 1)
        for j in range(early, n_blocks):
            finish(j)
        for j in range(n_blocks):
            final_copy(j, other).wait_recv()

        def drain():
            for j in range(n_blocks):
                pair_copy(j).wait_send()
                x_copy(j).wait_send()
                final_copy(j, mine).wait_send()

        return drain

    drain_first = branch_sum(0, tok_ref)

    norm_rows(res.at[0], gainm_ref)
    for off in range(1, n_tp):
        for s in range(n):
            pool_copy(off, s, lax.rem(t - off + n_tp, n_tp)).wait_recv()
    group_width = width // groups
    row_id = lax.broadcasted_iota(jnp.int32, (n_rows, n_rows), 0)
    col_id = lax.broadcasted_iota(jnp.int32, (n_rows, n_rows), 1)
    position = lax.broadcasted_iota(jnp.int32, (n_rows, 1), 0)
    for k, span in enumerate(pool_spans):
        low = row_id - span // 2
        band = jnp.where((col_id >= low) & (col_id < low + span), 1.0, 0.0).astype(jnp.bfloat16)
        first = jnp.maximum(position - span // 2, 0)
        last = jnp.minimum(position - span // 2 + span, n_rows)
        inverse = 1.0 / (last - first).astype(f32)
        cols = pl.ds(k * group_width, group_width)
        mean = jnp.dot(band, normed[:, cols], preferred_element_type=f32) * inverse
        deviation = (mean - normed[:, cols].astype(f32)).astype(jnp.bfloat16)
        mapped = jnp.dot(deviation, pool_full[k], preferred_element_type=f32) + bias_ref[pl.ds(k, 1), :]
        amix[:, cols] = (res[0, :, cols].astype(f32) + mapped * scale_ref[:, cols]).astype(jnp.bfloat16)

    norm_rows(amix, gain2_ref)

    @pl.loop(0, f_loc // tile)
    def _(i):
        cols = pl.ds(pl.multiple_of(i * tile, tile), tile)
        gate_proj = jnp.dot(normed[...], gu_full[0, :, cols], preferred_element_type=f32)
        up_proj = jnp.dot(normed[...], gu_full[1, :, cols], preferred_element_type=f32)
        hidden[:, cols] = activate(gate_proj, up_proj)

    drain_second = branch_sum(1, amix)
    out_copy = pltpu.make_async_copy(res.at[1], out_ref, osem)
    out_copy.start()

    for k in range(n_pieces):

        @pl.when(z < n - 1)
        def _():
            own_right(k).wait_send()

        @pl.when(z > 0)
        def _():
            own_left(k).wait_send()

    @pl.loop(1, n)
    def _(d):
        for k in range(n_pieces):

            def act(s, more, dev):
                @pl.when(more)
                def _():
                    pass_on(k, s, dev).wait_send()

                share(k, s, g).wait_send()

            both_sides(d, act)

    @pl.loop(0, n)
    def _(s):
        for off in range(1, n_tp):
            pool_copy(off, s, t).wait_send()

    drain_first()
    drain_second()
    out_copy.wait()


def fused_shards(
    n, n_tp, tokens, gate_weight, up_weight, down_weight, pool_weight, pool_bias, pool_scale,
    gain_first, gain_mix, gain_second,
):
    n_rows, width = tokens.shape
    d_loc, f_loc = gate_weight.shape
    groups = pool_weight.shape[1]
    pool = jnp.swapaxes(pool_weight, 0, 1)
    bf16, dma, vmem = jnp.bfloat16, pltpu.SemaphoreType.DMA, pltpu.VMEM
    in_vmem, anywhere = pl.BlockSpec(memory_space=pltpu.VMEM), pl.BlockSpec(memory_space=pl.ANY)
    half = n_rows // 2
    return pl.pallas_call(
        functools.partial(fused_kernel, (n, n_tp)),
        out_shape=jax.ShapeDtypeStruct((n_rows, width), bf16),
        in_specs=[in_vmem] + [anywhere] * 4 + [in_vmem] * 5,
        out_specs=anywhere,
        scratch_shapes=[
            vmem((2, n * d_loc, f_loc), bf16),
            vmem((n, 2, f_loc, d_loc // 2), bf16),
            vmem((groups, n * pool.shape[1], n_tp * pool.shape[2]), bf16),
            vmem((2, n_rows, f_loc), jnp.float32),
            vmem((n_rows, width), bf16),
            vmem((n_rows, f_loc), bf16),
            vmem((n_rows, width), bf16),
            vmem((2, n_rows, width), bf16),
            vmem((2, 2 * n, n_rows, d_loc // 2), bf16),
            vmem((2, 2 * n, half, d_loc // 2), bf16),
            vmem((2, 2 * n, half, d_loc // 2), bf16),
            vmem((2, 2 * n, half, d_loc // 2), bf16),
            dma((n, 13)), dma((13,)), dma((n, 13)), dma((n, 13)), dma((n, 13)),
            dma((n_tp - 1, n)), dma((n_tp - 1, n)), dma((5,)),
            *[dma((2, 2 * n))] * 6, dma,
        ],
        compiler_params=pltpu.CompilerParams(
            collective_id=0, has_side_effects=True, vmem_limit_bytes=60 * 1024 * 1024
        ),
    )(
        tokens, gate_weight, up_weight, down_weight, pool, pool_bias, pool_scale.reshape(1, width),
        gain_first.reshape(1, width), gain_mix.reshape(1, width), gain_second.reshape(1, width),
    )


def layer(n_grp, n, n_tp, *args):
    n_rows, width = args[0].shape
    d_loc, f_loc = args[1].shape
    pool_rows, _, pool_cols = args[4].shape
    fits = n_grp == 2 and n_tp == 4 and n % 2 == 0 and n <= 4 and n_rows % 64 == 0
    fits = fits and d_loc % 512 == 0 and f_loc % 256 == 0 and pool_rows % 32 == 0 and pool_cols % 128 == 0
    return fused_shards(n, n_tp, *args) if fits else shards(*args)


def solution(mesh):
    return jax.shard_map(
        functools.partial(layer, mesh.shape["grp"], mesh.shape["fs"], mesh.shape["tp"]),
        mesh=mesh,
        in_specs=(
            P(("grp", "fs"), None),
            P("fs", "tp"),
            P("fs", "tp"),
            P("tp", "fs"),
            P("fs", None, "tp"),
            P(),
            P(),
            P(),
            P(),
            P(),
        ),
        out_specs=P(("grp", "fs"), None),
        check_vma=False,
    )
```

```python
import functools

import jax
import jax.numpy as jnp
from jax import lax
from jax.experimental import pallas as pl
from jax.experimental.pallas import tpu as pltpu
from jax.sharding import PartitionSpec as P

eps = 1e-06
pool_spans = (2, 4, 8, 16)
pad_width = 8
MESH = pl.DeviceIdType.MESH


def rms_scale(values, gain_vec):
    fvalues = values.astype(jnp.float32)
    scaled = fvalues * lax.rsqrt(jnp.mean(fvalues * fvalues, axis=-1, keepdims=True) + eps)
    return (scaled * gain_vec).astype(jnp.bfloat16)


def ffn_hidden(normed, gate_full, up_full):
    gate_proj = jnp.dot(normed, gate_full, preferred_element_type=jnp.float32)
    up_proj = jnp.dot(normed, up_full, preferred_element_type=jnp.float32)
    return (jax.nn.silu(gate_proj) * up_proj).astype(jnp.bfloat16)


def pool_block(padded, offset, seq_len, pool_full, pool_bias, pool_scale):
    n_tokens = padded.shape[0] - 2 * pad_width
    group_width = pool_full.shape[0]
    position = offset + lax.iota(jnp.int32, n_tokens)
    column_pos = offset - pad_width + lax.iota(jnp.int32, padded.shape[0])
    center = padded[pad_width : pad_width + n_tokens].astype(jnp.float32)
    outputs = []
    for group_number, window_span in enumerate(pool_spans):
        low_edge = jnp.clip(position - window_span // 2, 0, seq_len)
        high_edge = jnp.clip(position - window_span // 2 + window_span, 0, seq_len)
        band_mask = (
            (column_pos[None, :] >= low_edge[:, None]) & (column_pos[None, :] < high_edge[:, None])
        ).astype(jnp.bfloat16)
        lower_col = group_number * group_width
        columns = padded[:, lower_col : lower_col + group_width]
        window_sum = jnp.dot(band_mask, columns, preferred_element_type=jnp.float32)
        window_mean = window_sum / (high_edge - low_edge).astype(jnp.float32)[:, None]
        deviation = (window_mean - center[:, lower_col : lower_col + group_width]).astype(
            jnp.bfloat16
        )
        mapped = jnp.dot(
            deviation, pool_full[:, group_number, :], preferred_element_type=jnp.float32
        )
        outputs.append(mapped + pool_bias[group_number])
    return jnp.concatenate(outputs, axis=-1) * pool_scale


def shards(
    tokens,
    gate_weight,
    up_weight,
    down_weight,
    pool_weight,
    pool_bias,
    pool_scale,
    gain_first,
    gain_mix,
    gain_second,
):
    gate_full, up_full, pool_half = (
        lax.all_gather(gate_weight, "fs", axis=0, tiled=True),
        lax.all_gather(up_weight, "fs", axis=0, tiled=True),
        lax.all_gather(pool_weight, "fs", axis=0, tiled=True),
    )
    down_full = lax.all_gather(down_weight, "fs", axis=1, tiled=True)
    pool_full = lax.all_gather(pool_half, "tp", axis=2, tiled=True)
    seq_len = tokens.shape[0]
    first_normed = rms_scale(tokens, gain_first)
    first_hidden = ffn_hidden(first_normed, gate_full, up_full)
    second_gate, second_up, second_down = (gate_full, up_full, down_full)
    first_branch = lax.psum(
        jnp.dot(first_hidden, down_full, preferred_element_type=jnp.float32).astype(jnp.bfloat16),
        "tp",
    ).astype(jnp.float32)
    after_first = (tokens.astype(jnp.float32) + 0.5 * first_branch).astype(jnp.bfloat16)
    mix_normed = rms_scale(after_first, gain_mix)
    padded = jnp.pad(mix_normed, ((pad_width, pad_width), (0, 0)))
    mixed = pool_block(padded, 0, seq_len, pool_full, pool_bias, pool_scale)
    after_mix = (after_first.astype(jnp.float32) + mixed).astype(jnp.bfloat16)
    second_normed = rms_scale(after_mix, gain_second)
    second_hidden = ffn_hidden(second_normed, second_gate, second_up)
    second_branch = lax.psum(
        jnp.dot(second_hidden, second_down, preferred_element_type=jnp.float32).astype(
            jnp.bfloat16
        ),
        "tp",
    ).astype(jnp.float32)
    return (after_mix.astype(jnp.float32) + 0.5 * second_branch).astype(jnp.bfloat16)


def fused_kernel(
    sizes, tok_ref, gate_ref, up_ref, down_ref, pool_ref, bias_ref, scale_ref, gain1_ref, gainm_ref, gain2_ref,
    out_ref,
    gu_full, down_full, pool_full, acc, normed, hidden, amix, res, part, rbuf, xs, xr,
    zsend, zleft, zrecv, ysend, yrecv, tsend, trecv, lsem, csend, crecv, xsend, xrecv, fsend, frecv, osem,
):
    n, n_tp = sizes
    g, z, t = lax.axis_index("grp"), lax.axis_index("fs"), lax.axis_index("tp")
    core = lax.rem(t, 2)
    y_peer, right, left = {"grp": 1 - g}, {"fs": z + 1}, {"fs": z - 1}
    mate, x_peer = {"tp": t + 1 - 2 * core}, {"tp": lax.rem(t + 2, n_tp)}
    n_rows, width = tok_ref.shape
    d_loc, f_loc = gate_ref.shape
    groups, pool_rows, pool_cols = pool_ref.shape
    half_rows = n_rows // 2
    block_cols = d_loc // 2
    f32 = jnp.float32

    def remote(src, dst, s_sem, r_sem, dev):
        return pltpu.make_async_remote_copy(
            src_ref=src, dst_ref=dst, send_sem=s_sem, recv_sem=r_sem, device_id=dev, device_id_type=MESH
        )

    barrier = pltpu.get_barrier_semaphore()

    def greet(dev):
        pl.semaphore_signal(barrier, inc=1, device_id=dev, device_id_type=MESH)

    greet(y_peer)
    for off in range(1, n_tp):
        greet({"tp": lax.rem(t + off, n_tp)})

    @pl.when(z > 0)
    def _():
        greet(left)

    @pl.when(z < n - 1)
    def _():
        greet(right)

    pl.semaphore_wait(barrier, n_tp + jnp.minimum(z, 1) + jnp.minimum(n - 1 - z, 1))

    pieces = [("pool", 0, 1)] + [(name, c, 4) for name in ("gate", "up", "down") for c in range(4)]
    n_pieces = len(pieces)

    def rows_of(name, half, c, count):
        if name == "down":
            return c * (f_loc // count), f_loc // count, f_loc
        total = {"pool": pool_rows, "gate": d_loc, "up": d_loc}[name]
        size = total // (2 * count)
        return half * (total // 2) + c * size, size, total

    def region(name, s, half, c, count):
        start, size, total = rows_of(name, half, c, count)
        if name == "down":
            return down_full.at[s, half, pl.ds(start, size), :]
        rows = pl.ds(pl.multiple_of(s * total + start, 16), size)
        if name == "pool":
            return pool_full.at[:, rows, pl.ds(pl.multiple_of(t * pool_cols, 128), pool_cols)]
        return gu_full.at[0 if name == "gate" else 1, rows, :]

    def source(name, half, c, count):
        start, size, _ = rows_of(name, half, c, count)
        if name == "down":
            return down_ref.at[pl.ds(start, size), pl.ds(pl.multiple_of(half * block_cols, 128), block_cols)]
        rows = pl.ds(pl.multiple_of(start, 16), size)
        if name == "pool":
            return pool_ref.at[:, rows, :]
        return {"gate": gate_ref, "up": up_ref}[name].at[rows, :]

    def own_right(k):
        name, c, count = pieces[k]
        return remote(source(name, g, c, count), region(name, z, g, c, count), zsend.at[z, k], zrecv.at[z, k], right)

    def own_left(k):
        name, c, count = pieces[k]
        return remote(source(name, g, c, count), region(name, z, g, c, count), zleft.at[k], zrecv.at[z, k], left)

    def pass_on(k, s, dev):
        name, c, count = pieces[k]
        there = region(name, s, g, c, count)
        return remote(there, there, zsend.at[s, k], zrecv.at[s, k], dev)

    def share(k, s, half):
        name, c, count = pieces[k]
        there = region(name, s, half, c, count)
        return remote(there, there, ysend.at[s, k], yrecv.at[s, k], y_peer)

    for k in range(n_pieces):

        @pl.when(z < n - 1)
        def _():
            own_right(k).start()

        @pl.when(z > 0)
        def _():
            own_left(k).start()

    own_rows = pl.ds(pl.multiple_of(z * d_loc, 128), d_loc)
    own_pool = pool_full.at[
        :, pl.ds(pl.multiple_of(z * pool_rows, 16), pool_rows), pl.ds(pl.multiple_of(t * pool_cols, 128), pool_cols)
    ]
    local = [
        pltpu.make_async_copy(pool_ref, own_pool, lsem.at[0]),
        pltpu.make_async_copy(gate_ref, gu_full.at[0, own_rows, :], lsem.at[1]),
        pltpu.make_async_copy(up_ref, gu_full.at[1, own_rows, :], lsem.at[2]),
        pltpu.make_async_copy(down_ref.at[:, pl.ds(0, block_cols)], down_full.at[z, 0], lsem.at[3]),
        pltpu.make_async_copy(down_ref.at[:, pl.ds(block_cols, block_cols)], down_full.at[z, 1], lsem.at[4]),
    ]
    for copy in local:
        copy.start()

    def norm_rows(src, gain):
        @pl.loop(0, n_rows // 32)
        def _(r):
            rows = pl.ds(pl.multiple_of(r * 32, 32), 32)
            values = src[rows, :].astype(f32)
            scaled = values * lax.rsqrt(jnp.mean(values * values, axis=-1, keepdims=True) + eps)
            normed[rows, :] = (scaled * gain[...]).astype(jnp.bfloat16)

    tile = 256

    def add_shard(w, s):
        k_cols = pl.ds(pl.multiple_of(s * d_loc, 128), d_loc)

        @pl.loop(0, f_loc // tile)
        def _(i):
            cols = pl.ds(pl.multiple_of(i * tile, tile), tile)
            acc[w, :, cols] += jnp.dot(normed[:, k_cols], gu_full[w, k_cols, cols], preferred_element_type=f32)

    def pool_copy(off, s, sender):
        cols = pl.ds(pl.multiple_of(sender * pool_cols, 128), pool_cols)
        there = pool_full.at[:, pl.ds(pl.multiple_of(s * pool_rows, 16), pool_rows), cols]
        return remote(there, there, tsend.at[off - 1, s], trecv.at[off - 1, s], {"tp": lax.rem(t + off, n_tp)})

    def spread_pool(s):
        for off in range(1, n_tp):
            pool_copy(off, s, t).start()

    norm_rows(tok_ref, gain1_ref)
    acc[...] = jnp.zeros_like(acc)
    for copy in local:
        copy.wait()
    spread_pool(z)

    @pl.loop(0, 2)
    def _(w):
        add_shard(w, z)

    def both_sides(d, act):
        @pl.when(z >= d)
        def _():
            act(z - d, z < n - 1, right)

        @pl.when(z + d < n)
        def _():
            act(z + d, z > 0, left)

    def relay(name, d, only=None):
        for k in range(n_pieces):
            if pieces[k][0] != name or only not in (None, pieces[k][1]):
                continue

            def act(s, more, dev):
                pass_on(k, s, dev).wait_recv()

                @pl.when(more)
                def _():
                    pass_on(k, s, dev).start()

                share(k, s, g).start()

            both_sides(d, act)

    def settle(name, s):
        for k in range(n_pieces):
            if pieces[k][0] == name:
                share(k, s, 1 - g).wait_recv()

    def settle_pool(s, *_):
        settle("pool", s)
        spread_pool(s)

    def settle_gate(s, *_):
        settle("gate", s)
        add_shard(0, s)

    def settle_up(s, *_):
        settle("up", s)
        add_shard(1, s)

    @pl.loop(1, n - 1)
    def _(d):
        relay("pool", d)
        relay("gate", d)
        both_sides(d, settle_pool)
        relay("up", d)
        both_sides(d, settle_gate)
        relay("down", d)
        both_sides(d, settle_up)

    relay("pool", n - 1)
    relay("gate", n - 1)
    both_sides(n - 1, settle_pool)
    relay("up", n - 1)
    both_sides(n - 1, settle_gate)
    both_sides(n - 1, settle_up)
    relay("down", n - 1, 0)

    def activate(gate_proj, up_proj):
        return (gate_proj / (1.0 + jnp.exp(-gate_proj)) * up_proj).astype(jnp.bfloat16)

    @pl.loop(0, f_loc // tile)
    def _(i):
        cols = pl.ds(pl.multiple_of(i * tile, tile), tile)
        hidden[:, cols] = activate(acc[0, :, cols], acc[1, :, cols])

    turn = 1 - 2 * ((2 * z) // n)
    mine = pl.ds(pl.multiple_of(core * half_rows, 16), half_rows)
    other = pl.ds(pl.multiple_of((1 - core) * half_rows, 16), half_rows)

    n_blocks = 2 * n

    def branch_sum(phase, base):
        def place(j):
            return lax.rem(z + turn * (j // 2) + n, n), g if j % 2 == 0 else 1 - g

        def columns(j):
            s, half = place(j)
            return pl.ds(pl.multiple_of(s * d_loc + half * block_cols, 128), block_cols)

        def pair_copy(j):
            return remote(part.at[phase, j, other, :], rbuf.at[phase, j], csend.at[phase, j], crecv.at[phase, j], mate)

        def x_copy(j):
            return remote(xs.at[phase, j], xr.at[phase, j], xsend.at[phase, j], xrecv.at[phase, j], x_peer)

        def final_copy(j, rows):
            there = res.at[phase, rows, columns(j)]
            return remote(there, there, fsend.at[phase, j], frecv.at[phase, j], mate)

        def multiply(j):
            s, half = place(j)
            if phase == 0 and j in (1, 3, 5):
                relay("down", n - 1, (j + 1) // 2)
            if phase == 0 and j >= 2 and j % 2 == 1:
                settle("down", s)
            part[phase, j] = jnp.dot(
                hidden[...], down_full[s, half], preferred_element_type=f32
            ).astype(jnp.bfloat16)
            pair_copy(j).start()

        def add_pair(j):
            pair_copy(j).wait_recv()
            xs[phase, j] = (part[phase, j, mine, :].astype(f32) + rbuf[phase, j].astype(f32)).astype(jnp.bfloat16)
            x_copy(j).start()

        def finish(j):
            x_copy(j).wait_recv()
            total = xs[phase, j].astype(f32) + xr[phase, j].astype(f32)
            cols = columns(j)
            res[phase, mine, cols] = (base[mine, cols].astype(f32) + 0.5 * total).astype(jnp.bfloat16)
            final_copy(j, mine).start()

        early = n_blocks // 2 if phase == 0 else 0
        for j in range(n_blocks + 1):
            if j == n_blocks - 1:
                for done in range(early):
                    finish(done)
            if j < n_blocks:
                multiply(j)
            if j > 0:
                add_pair(j - 1)
        for j in range(early, n_blocks):
            finish(j)
        for j in range(n_blocks):
            final_copy(j, other).wait_recv()

        def drain():
            for j in range(n_blocks):
                pair_copy(j).wait_send()
                x_copy(j).wait_send()
                final_copy(j, mine).wait_send()

        return drain

    drain_first = branch_sum(0, tok_ref)

    norm_rows(res.at[0], gainm_ref)
    for off in range(1, n_tp):
        for s in range(n):
            pool_copy(off, s, lax.rem(t - off + n_tp, n_tp)).wait_recv()
    group_width = width // groups
    row_id = lax.broadcasted_iota(jnp.int32, (n_rows, n_rows), 0)
    col_id = lax.broadcasted_iota(jnp.int32, (n_rows, n_rows), 1)
    position = lax.broadcasted_iota(jnp.int32, (n_rows, 1), 0)
    for k, span in enumerate(pool_spans):
        low = row_id - span // 2
        band = jnp.where((col_id >= low) & (col_id < low + span), 1.0, 0.0).astype(jnp.bfloat16)
        first = jnp.maximum(position - span // 2, 0)
        last = jnp.minimum(position - span // 2 + span, n_rows)
        inverse = 1.0 / (last - first).astype(f32)
        cols = pl.ds(k * group_width, group_width)
        mean = jnp.dot(band, normed[:, cols], preferred_element_type=f32) * inverse
        deviation = (mean - normed[:, cols].astype(f32)).astype(jnp.bfloat16)
        mapped = jnp.dot(deviation, pool_full[k], preferred_element_type=f32) + bias_ref[pl.ds(k, 1), :]
        amix[:, cols] = (res[0, :, cols].astype(f32) + mapped * scale_ref[:, cols]).astype(jnp.bfloat16)

    norm_rows(amix, gain2_ref)

    @pl.loop(0, f_loc // tile)
    def _(i):
        cols = pl.ds(pl.multiple_of(i * tile, tile), tile)
        gate_proj = jnp.dot(normed[...], gu_full[0, :, cols], preferred_element_type=f32)
        up_proj = jnp.dot(normed[...], gu_full[1, :, cols], preferred_element_type=f32)
        hidden[:, cols] = activate(gate_proj, up_proj)

    drain_second = branch_sum(1, amix)
    out_copy = pltpu.make_async_copy(res.at[1], out_ref, osem)
    out_copy.start()

    for k in range(n_pieces):

        @pl.when(z < n - 1)
        def _():
            own_right(k).wait_send()

        @pl.when(z > 0)
        def _():
            own_left(k).wait_send()

    @pl.loop(1, n)
    def _(d):
        for k in range(n_pieces):

            def act(s, more, dev):
                @pl.when(more)
                def _():
                    pass_on(k, s, dev).wait_send()

                share(k, s, g).wait_send()

            both_sides(d, act)

    @pl.loop(0, n)
    def _(s):
        for off in range(1, n_tp):
            pool_copy(off, s, t).wait_send()

    drain_first()
    drain_second()
    out_copy.wait()


def fused_shards(
    n, n_tp, tokens, gate_weight, up_weight, down_weight, pool_weight, pool_bias, pool_scale,
    gain_first, gain_mix, gain_second,
):
    n_rows, width = tokens.shape
    d_loc, f_loc = gate_weight.shape
    groups = pool_weight.shape[1]
    pool = jnp.swapaxes(pool_weight, 0, 1)
    bf16, dma, vmem = jnp.bfloat16, pltpu.SemaphoreType.DMA, pltpu.VMEM
    in_vmem, anywhere = pl.BlockSpec(memory_space=pltpu.VMEM), pl.BlockSpec(memory_space=pl.ANY)
    half = n_rows // 2
    return pl.pallas_call(
        functools.partial(fused_kernel, (n, n_tp)),
        out_shape=jax.ShapeDtypeStruct((n_rows, width), bf16),
        in_specs=[in_vmem] + [anywhere] * 4 + [in_vmem] * 5,
        out_specs=anywhere,
        scratch_shapes=[
            vmem((2, n * d_loc, f_loc), bf16),
            vmem((n, 2, f_loc, d_loc // 2), bf16),
            vmem((groups, n * pool.shape[1], n_tp * pool.shape[2]), bf16),
            vmem((2, n_rows, f_loc), jnp.float32),
            vmem((n_rows, width), bf16),
            vmem((n_rows, f_loc), bf16),
            vmem((n_rows, width), bf16),
            vmem((2, n_rows, width), bf16),
            vmem((2, 2 * n, n_rows, d_loc // 2), bf16),
            vmem((2, 2 * n, half, d_loc // 2), bf16),
            vmem((2, 2 * n, half, d_loc // 2), bf16),
            vmem((2, 2 * n, half, d_loc // 2), bf16),
            dma((n, 13)), dma((13,)), dma((n, 13)), dma((n, 13)), dma((n, 13)),
            dma((n_tp - 1, n)), dma((n_tp - 1, n)), dma((5,)),
            *[dma((2, 2 * n))] * 6, dma,
        ],
        compiler_params=pltpu.CompilerParams(
            collective_id=0, has_side_effects=True, vmem_limit_bytes=60 * 1024 * 1024
        ),
    )(
        tokens, gate_weight, up_weight, down_weight, pool, pool_bias, pool_scale.reshape(1, width),
        gain_first.reshape(1, width), gain_mix.reshape(1, width), gain_second.reshape(1, width),
    )


def layer(n_grp, n, n_tp, *args):
    n_rows, width = args[0].shape
    d_loc, f_loc = args[1].shape
    pool_rows, _, pool_cols = args[4].shape
    fits = n_grp == 2 and n_tp == 4 and n % 2 == 0 and n <= 4 and n_rows % 64 == 0
    fits = fits and d_loc % 512 == 0 and f_loc % 256 == 0 and pool_rows % 32 == 0 and pool_cols % 128 == 0
    return fused_shards(n, n_tp, *args) if fits else shards(*args)


def solution(mesh):
    return jax.shard_map(
        functools.partial(layer, mesh.shape["grp"], mesh.shape["fs"], mesh.shape["tp"]),
        mesh=mesh,
        in_specs=(
            P(("grp", "fs"), None),
            P("fs", "tp"),
            P("fs", "tp"),
            P("tp", "fs"),
            P("fs", None, "tp"),
            P(),
            P(),
            P(),
            P(),
            P(),
        ),
        out_specs=P(("grp", "fs"), None),
        check_vma=False,
    )
```
